32 devices in a mesh: rep: 2 (over x), fs: 8 (over z, y), tp: 2 (over core).
Axes of the slice: x: 2, y: 2, z: 4, core: 2. Of those that a mesh axis runs over, the one named last changes fastest.
Arguments:
- tokens: bfloat16 [16384, 2048], P(('rep', 'fs', 'tp')), parts along dimension 0, may hold values from -6 to 6
- mix_gain: float32 [2048], replicated, may hold values from 0.1 to 1.9
- w_query: bfloat16 [2048, 512], P('fs', 'tp'), may hold values from -0.125 to 0.125
- w_key: bfloat16 [2048, 512], P('fs', 'tp'), may hold values from -0.125 to 0.125
- w_value: bfloat16 [2048, 1024], P('fs', 'tp'), may hold values from -0.125 to 0.125
- w_out: bfloat16 [1024, 2048], P('tp', 'fs'), may hold values from -0.1875 to 0.1875
- ffn_gain: float32 [2048], replicated, may hold values from 0.1 to 1.9
- w_ffgate: bfloat16 [2048, 2816], P('fs', 'tp'), may hold values from -0.125 to 0.125
- w_ffup: bfloat16 [2048, 2816], P('fs', 'tp'), may hold values from -0.125 to 0.125
- conv_gate: float32 [3, 2816], replicated, may hold values from -3 to 3
- conv_up: float32 [3, 2816], replicated, may hold values from -3 to 3
- w_down: bfloat16 [2816, 2048], P('tp', 'fs'), may hold values from -0.109375 to 0.109375
Outputs:
- layer_out: bfloat16 [16384, 2048], P(('rep', 'fs', 'tp')), parts along dimension 0
The draws below stay inside these ranges and needn't reach their ends.
There are 2 independent parts, one for each index of `rep`. The reference program is written for one: setup_inputs(seed, part) draws one part's arguments, and reference() takes and returns one part's arrays. A program takes and returns all parts, laid end to end along the dimension named above; an argument that names none is the same for every part. Nothing has to cross between parts.
All inputs are finite; a program needn't handle non-finite values.
Results may differ from the reference program's by a relative error of at most 0.014.
Values may be sent and summed in bfloat16 or wider, within the bound.
A program may use at most 128 MiB of HBM per device.

```python
import jax
import jax.numpy as jnp
from jax import lax

D = 2048
HEADS = 4
DK = 128
DV = 256
FF = 2816
KERNEL = 3
BLOCK = 128
LENGTH = 1024
TOKENS = 8192
N_TP = 2


def levels(key, shape, split, low, largest):
    level, own = 1.0, jax.random.fold_in(key, 6)
    for position, shards_of in split:
        draws = jnp.exp(jax.random.uniform(jax.random.fold_in(own, position), (shards_of,), jnp.float32, low / len(split), largest / len(split)))
        level = level * jnp.repeat(draws, shape[position] // shards_of).reshape([-1 if axis == position else 1 for axis in range(len(shape))])
    return level


def bell_draw(key, dims, scale, most, shards=(), kind=jnp.bfloat16):
    level = levels(key, dims, shards, -0.22, 0.18) if shards else 1.0
    drawn = jax.random.normal(key, dims, jnp.float32) * scale * level
    return jnp.minimum(jnp.maximum(drawn, -most), most).astype(kind)


def setup_inputs(seed: int = 0, part: int = 0) -> dict:
    arg_keys = jax.random.split(jax.random.key(seed), 13)
    part_keys = jax.random.split(jax.random.fold_in(arg_keys[12], part), 13)
    return {
        "tokens": bell_draw(part_keys[0], (TOKENS, D), 1.0, 6.0, ((0, 16),)),
        "mix_gain": jnp.clip(1.0 + 0.18 * jax.random.normal(arg_keys[1], (D,), jnp.float32), 0.1, 1.9),
        "w_query": bell_draw(arg_keys[2], (D, HEADS * DK), D ** -0.5, 0.125, ((0, 8), (1, 2))),
        "w_key": bell_draw(arg_keys[3], (D, HEADS * DK), D ** -0.5, 0.125, ((0, 8), (1, 2))),
        "w_value": bell_draw(arg_keys[4], (D, HEADS * DV), D ** -0.5, 0.125, ((0, 8), (1, 2))),
        "w_out": bell_draw(arg_keys[5], (HEADS * DV, D), (HEADS * DV) ** -0.5, 0.1875, ((0, 2), (1, 8))),
        "ffn_gain": jnp.clip(1.0 + 0.18 * jax.random.normal(arg_keys[6], (D,), jnp.float32), 0.1, 1.9),
        "w_ffgate": bell_draw(arg_keys[7], (D, FF), D ** -0.5, 0.125, ((0, 8), (1, 2))),
        "w_ffup": bell_draw(arg_keys[8], (D, FF), D ** -0.5, 0.125, ((0, 8), (1, 2))),
        "conv_gate": bell_draw(arg_keys[9], (KERNEL, FF), 0.58, 3.0, (), jnp.float32),
        "conv_up": bell_draw(arg_keys[10], (KERNEL, FF), 0.58, 3.0, (), jnp.float32),
        "w_down": bell_draw(arg_keys[11], (FF, D), FF ** -0.5, 0.109375, ((0, 2), (1, 8))),
    }


epsilon = 1e-06

def rms_rows(matrix, scale_vec):
    values = matrix.astype(jnp.float32)
    factor = lax.rsqrt(lax.optimization_barrier(jnp.mean(values * values, axis=-1, keepdims=True)) + epsilon)
    return (values * factor * scale_vec).astype(jnp.bfloat16)

def rotate_heads(matrix):
    length = matrix.shape[0]
    half_width = matrix.shape[-1] // 2
    inverse = 10000.0 ** (-jnp.arange(half_width, dtype=jnp.float32) * 2.0 / (2 * half_width))
    angles = jnp.arange(length, dtype=jnp.float32)[:, None] * inverse[None, :]
    cosine = jnp.cos(angles)[:, None, :]
    sine = jnp.sin(angles)[:, None, :]
    values = matrix.astype(jnp.float32)
    first_half = values[..., :half_width]
    second_half = values[..., half_width:]
    return jnp.concatenate([first_half * cosine - second_half * sine, first_half * sine + second_half * cosine], axis=-1)

def retain_blocks(rot_query, rot_key, value, rates, block_len):
    length, head_count, width_k = rot_query.shape
    width_v = value.shape[-1]
    blocks = length // block_len
    query4 = rot_query.reshape(blocks, block_len, head_count, width_k).astype(jnp.float32)
    key4 = rot_key.reshape(blocks, block_len, head_count, width_k)
    value4 = value.reshape(blocks, block_len, head_count, width_v).astype(jnp.float32)
    places = jnp.arange(block_len, dtype=jnp.float32)
    spacing = places[:, None] - places[None, :]
    inside = jnp.where(spacing[None] >= 0, jnp.exp(-jnp.maximum(spacing, 0.0)[None] * rates[:, None, None]), 0.0)
    scores = jnp.einsum('cihd,cjhd->chij', query4, key4.astype(jnp.float32), precision=lax.Precision.HIGHEST)
    weights = (scores * inside[None]).astype(jnp.bfloat16)
    inner_part = jnp.einsum('chij,cjhe->cihe', weights.astype(jnp.float32), value4, precision=lax.Precision.HIGHEST)
    tail_decay = jnp.exp(-(block_len - 1.0 - places)[:, None] * rates[None, :])
    decayed = (key4.astype(jnp.float32) * tail_decay[None, :, :, None]).astype(jnp.bfloat16)
    states = jnp.einsum('cjhd,cjhe->chde', decayed.astype(jnp.float32), value4, precision=lax.Precision.HIGHEST)
    passing = jnp.exp(-block_len * rates)[:, None, None]

    def advance(carried, fresh):
        return (carried * passing + fresh, carried)
    _, before = lax.scan(advance, jnp.zeros((head_count, width_k, width_v), jnp.float32), states)
    onset_decay = jnp.exp(-(places + 1.0)[:, None] * rates[None, :])
    cross_part = jnp.einsum('cihd,chde->cihe', query4, before, precision=lax.Precision.HIGHEST) * onset_decay[None, :, :, None]
    return (inner_part + cross_part).reshape(length, head_count, width_v)

def head_norm(retained):
    average = lax.optimization_barrier(jnp.mean(retained, axis=-1, keepdims=True))
    centered = retained - average
    return centered * lax.rsqrt(lax.optimization_barrier(jnp.mean(centered * centered, axis=-1, keepdims=True)) + epsilon)

def group_sum(hidden, weight):
    width = hidden.shape[1] // N_TP
    total = jnp.zeros((hidden.shape[0], weight.shape[1]), jnp.float32)
    for section in range(N_TP):
        partial_sum = jnp.dot(hidden[:, section * width:(section + 1) * width], weight[section * width:(section + 1) * width], preferred_element_type=jnp.float32).astype(jnp.bfloat16)
        partial_sum = lax.optimization_barrier(partial_sum)
        total = total + partial_sum.astype(jnp.float32)
    return total

def causal_taps(matrix, kernel_w):
    length = matrix.shape[0]
    padded = jnp.pad(matrix.astype(jnp.float32), ((KERNEL - 1, 0), (0, 0)))
    total = jnp.zeros((length, matrix.shape[1]), jnp.float32)
    for tap_idx in range(KERNEL):
        total = total + kernel_w[tap_idx][None, :] * padded[tap_idx:tap_idx + length]
    return total

def reference(tokens, mix_gain, w_query, w_key, w_value, w_out, ffn_gain, w_ffgate, w_ffup, conv_gate, conv_up, w_down):
    sequences = tokens.reshape(TOKENS // LENGTH, LENGTH, D)

    def layer(rows):
        normed = rms_rows(rows, mix_gain)
        query = jnp.dot(normed, w_query, preferred_element_type=jnp.float32).astype(jnp.bfloat16)
        key = jnp.dot(normed, w_key, preferred_element_type=jnp.float32).astype(jnp.bfloat16)
        value = jnp.dot(normed, w_value, preferred_element_type=jnp.float32).astype(jnp.bfloat16)
        rot_query = rotate_heads(query.reshape(LENGTH, HEADS, DK)).astype(jnp.bfloat16)
        rot_key = (rotate_heads(key.reshape(LENGTH, HEADS, DK)) * DK ** (-0.5)).astype(jnp.bfloat16)
        rates = 1.0 / 16.0 * (32.0 / LENGTH) ** (jnp.arange(HEADS, dtype=jnp.float32) / (HEADS - 1))
        retained = retain_blocks(rot_query, rot_key, value.reshape(LENGTH, HEADS, DV), rates, BLOCK)
        hidden = head_norm(retained).reshape(LENGTH, HEADS * DV).astype(jnp.bfloat16)
        mix_sum = group_sum(hidden, w_out)
        resid = (rows.astype(jnp.float32) + mix_sum).astype(jnp.bfloat16)
        normed_ffn = rms_rows(resid, ffn_gain)
        gate_pre = jnp.dot(normed_ffn, w_ffgate, preferred_element_type=jnp.float32).astype(jnp.bfloat16)
        up_pre = jnp.dot(normed_ffn, w_ffup, preferred_element_type=jnp.float32).astype(jnp.bfloat16)
        activ = (jax.nn.silu(causal_taps(gate_pre, conv_gate)) * causal_taps(up_pre, conv_up)).astype(jnp.bfloat16)
        ffn_sum = group_sum(activ, w_down)
        return (resid.astype(jnp.float32) + ffn_sum).astype(jnp.bfloat16)
    return lax.map(layer, sequences).reshape(TOKENS, D)
```

```python
import functools

import jax
import jax.numpy as jnp
from jax import lax
from jax.experimental import pallas as pl
from jax.experimental.pallas import tpu as pltpu
from jax.sharding import PartitionSpec as P

HEADS = 4
DK = 128
DV = 256
KERNEL = 3
BLOCK = 128
LENGTH = 1024
MESH = pl.DeviceIdType.MESH
ROWS, COLS = "rows", "cols"


epsilon = 1e-06


def gather_kernel(sizes, kinds, *refs):
    reps, fs, tps = sizes
    count = len(kinds)
    tokens = refs[0]
    shards = refs[1 : 1 + count]
    both = refs[1 + count]
    fulls = refs[2 + count : 2 + 2 * count]
    (tok_sems, own_sems, up_send, up_recv, down_send, down_recv, y_send, y_recv, x_send, x_recv) = refs[
        2 + 2 * count :
    ]
    depth = fs // 2
    rep = lax.axis_index("rep")
    place = lax.axis_index("fs")
    core = lax.axis_index("tp")
    z = place // 2
    y = lax.rem(place, 2)
    above = {"fs": lax.rem(place + 2, fs)}
    below = {"fs": lax.rem(place + fs - 2, fs)}
    beside = {"fs": z * 2 + 1 - y}
    twin = {"rep": 1 - rep}
    other = {"tp": 1 - core}

    barrier = pltpu.get_barrier_semaphore()

    def greet(device):
        pl.semaphore_signal(barrier, inc=1, device_id=device, device_id_type=MESH)

    greet(beside)
    greet(twin)
    greet(other)
    pl.when(z < depth - 1)(lambda: greet(above))
    pl.when(z > 0)(lambda: greet(below))
    at_end = (z == 0) | (z == depth - 1)
    pl.when(at_end)(lambda: pl.semaphore_wait(barrier, 4))
    pl.when(jnp.logical_not(at_end))(lambda: pl.semaphore_wait(barrier, 5))

    def slot(p, owner, start, size):
        rows, cols = shards[p].shape
        start = pl.multiple_of(start, 16)
        if kinds[p] == COLS:
            return fulls[p].at[pl.ds(start, size), pl.ds(pl.multiple_of(owner * cols, 128), cols)]
        return fulls[p].at[pl.ds(pl.multiple_of(owner * rows, 16) + start, size)]

    def spans(p):
        rows = shards[p].shape[0]
        third = rows * 5 // 16 // 16 * 16
        return third, rows - third

    def piece(p, owner, own):
        third, most = spans(p)
        start = rep * third
        src = shards[p].at[pl.ds(pl.multiple_of(start, 16), most)] if own else slot(p, owner, start, most)
        return src, slot(p, owner, start, most)

    def copy(src, dst, send, recv, device):
        return pltpu.make_async_remote_copy(
            src_ref=src, dst_ref=dst, send_sem=send, recv_sem=recv, device_id=device, device_id_type=MESH
        )

    def clip(value):
        return jnp.minimum(jnp.maximum(value, 0), depth - 1)

    def up(p, s):
        src, dst = piece(p, clip(z - s) * 2 + y, s == 0)
        return copy(src, dst, up_send.at[p, s], up_recv.at[p, s], above)

    def down(p, s):
        src, dst = piece(p, clip(z + s) * 2 + y, s == 0)
        return copy(src, dst, down_send.at[p, s], down_recv.at[p, s], below)

    def up_in(p, s):
        dst = piece(p, clip(z - 1 - s) * 2 + y, False)[1]
        return copy(dst, dst, up_send.at[p, s], up_recv.at[p, s], above)

    def down_in(p, s):
        dst = piece(p, clip(z + 1 + s) * 2 + y, False)[1]
        return copy(dst, dst, down_send.at[p, s], down_recv.at[p, s], below)

    def level(k):
        return z if k == 0 else (clip(z - k) if k < depth else clip(z + k - depth + 1))

    def valid(k):
        return z >= 0 if k == 0 else (z - k >= 0 if k < depth else z + k - depth + 1 < depth)

    def y_copy(p, k):
        src, dst = piece(p, level(k) * 2 + y, k == 0)
        return copy(src, dst, y_send.at[p, k], y_recv.at[p, k], beside)

    def y_in(p, k):
        dst = piece(p, level(k) * 2 + 1 - y, False)[1]
        return copy(dst, dst, y_send.at[p, k], y_recv.at[p, k], beside)

    kmax = 2 * depth - 1

    def x_copy(p, k, side, mine):
        third, most = spans(p)
        who = rep if mine else 1 - rep
        lane = y if side == 0 else 1 - y
        ref = slot(p, level(k) * 2 + lane, who * most, third)
        return copy(ref, ref, x_send.at[p, side * kmax + k], x_recv.at[p, side * kmax + k], twin)

    tok_rows = tokens.shape[0]
    here = both.at[pl.ds(pl.multiple_of(core * tok_rows, 16), tok_rows)]
    tok_out = copy(tokens, here, tok_sems.at[0], tok_sems.at[1], other)
    tok_out.start()
    tok_own = pltpu.make_async_copy(tokens, here, tok_sems.at[2])
    tok_own.start()
    owns = []
    for p in range(count):
        own = pltpu.make_async_copy(shards[p], slot(p, place, 0, shards[p].shape[0]), own_sems.at[p])
        own.start()
        owns.append(own)

    steps = depth - 1
    events = [(p, s) for p in range(count) for s in range(steps)]

    def start_z(p, s):
        pl.when((z - s >= 0) & (z < depth - 1))(lambda: up(p, s).start())
        pl.when((z + s <= depth - 1) & (z > 0))(lambda: down(p, s).start())
        if s == 0:
            y_copy(p, 0).start()

    def take_z(p, s):
        ku, kd = s + 1, depth + s

        @pl.when(z - 1 - s >= 0)
        def _():
            up_in(p, s).wait_recv()

        @pl.when(z + 1 + s <= depth - 1)
        def _():
            down_in(p, s).wait_recv()

    def spread(p, s):
        for k in (s + 1, depth + s):

            @pl.when(valid(k))
            def _():
                y_copy(p, k).start()
                x_copy(p, k, 0, True).start()

    def take_y(p, k):
        @pl.when(valid(k))
        def _():
            y_in(p, k).wait_recv()
            x_copy(p, k, 1, True).start()

    def finish_y(p, s):
        if s == 0:
            take_y(p, 0)
        take_y(p, s + 1)
        take_y(p, depth + s)

    lag = 2
    total = len(events)
    start_z(*events[0])
    for e in range(total + lag):
        if e < total:
            take_z(*events[e])
            if e + 1 < total:
                start_z(*events[e + 1])
            spread(*events[e])
        if e >= lag:
            finish_y(*events[e - lag])

    for p in range(count):
        for k in range(kmax):

            @pl.when(valid(k))
            def _():
                if k > 0:
                    x_copy(p, k, 0, False).wait_recv()
                    x_copy(p, k, 0, True).wait_send()
                x_copy(p, k, 1, False).wait_recv()
                x_copy(p, k, 1, True).wait_send()
                y_copy(p, k).wait_send()

        for s in range(steps):
            pl.when((z - s >= 0) & (z < depth - 1))(lambda: up(p, s).wait_send())
            pl.when((z + s <= depth - 1) & (z > 0))(lambda: down(p, s).wait_send())
    for own in owns:
        own.wait()
    tok_own.wait()
    tok_out.wait()


def gather_all(sizes, tokens, shards):
    fs = sizes[1]
    kinds = []
    outs = [jax.ShapeDtypeStruct((tokens.shape[0] * 2, tokens.shape[1]), tokens.dtype)]
    for shard, by_cols in shards:
        rows, cols = shard.shape
        side = by_cols and cols % 128 == 0
        kinds.append(COLS if side else ROWS)
        outs.append(jax.ShapeDtypeStruct((rows, cols * fs) if side else (rows * fs, cols), shard.dtype))
    count, depth = len(shards), fs // 2
    dma = pltpu.SemaphoreType.DMA
    vmem = pl.BlockSpec(memory_space=pltpu.VMEM)
    anywhere = pl.BlockSpec(memory_space=pl.ANY)
    got = pl.pallas_call(
        functools.partial(gather_kernel, sizes, tuple(kinds)),
        out_shape=outs,
        in_specs=[vmem] * (count + 1),
        out_specs=[anywhere] * (count + 1),
        scratch_shapes=[dma((3,)), dma((count,))]
        + [dma((count, depth - 1))] * 4
        + [dma((count, 2 * depth - 1))] * 2
        + [dma((count, 4 * depth - 2))] * 2,
        compiler_params=pltpu.CompilerParams(collective_id=0, has_side_effects=True),
    )(tokens, *[shard for shard, _ in shards])
    fulls = []
    for full, (shard, by_cols), kind in zip(got[1:], shards, kinds):
        if by_cols and kind == ROWS:
            rows, cols = shard.shape
            full = full.reshape(fs, rows, cols).transpose(1, 0, 2).reshape(rows, fs * cols)
        fulls.append(full)
    return got[0], fulls


def rms_rows(matrix, scale_vec):
    values = matrix.astype(jnp.float32)
    factor = lax.rsqrt(jnp.mean(values * values, axis=-1, keepdims=True) + epsilon)
    return (values * factor * scale_vec).astype(jnp.bfloat16)


def rotate_heads(matrix):
    length = matrix.shape[0]
    half_width = matrix.shape[-1] // 2
    inverse = 10000.0 ** (-jnp.arange(half_width, dtype=jnp.float32) * 2.0 / (2 * half_width))
    angles = jnp.arange(length, dtype=jnp.float32)[:, None] * inverse[None, :]
    cosine = jnp.cos(angles)[:, None, :]
    sine = jnp.sin(angles)[:, None, :]
    values = matrix.astype(jnp.float32)
    first_half = values[..., :half_width]
    second_half = values[..., half_width:]
    return jnp.concatenate(
        [first_half * cosine - second_half * sine, first_half * sine + second_half * cosine],
        axis=-1,
    )


def retain_blocks(rot_query, rot_key, value, rates, block_len):
    length, head_count, width_k = rot_query.shape
    width_v = value.shape[-1]
    blocks = length // block_len
    query4 = rot_query.reshape(blocks, block_len, head_count, width_k)
    key4 = rot_key.reshape(blocks, block_len, head_count, width_k)
    value4 = value.reshape(blocks, block_len, head_count, width_v)
    places = jnp.arange(block_len, dtype=jnp.float32)
    spacing = places[:, None] - places[None, :]
    inside = jnp.where(
        spacing[None] >= 0, jnp.exp(-jnp.maximum(spacing, 0.0)[None] * rates[:, None, None]), 0.0
    )
    scores = jnp.einsum("cihd,cjhd->chij", query4, key4, preferred_element_type=jnp.float32)
    weights = (scores * inside[None]).astype(jnp.bfloat16)
    inner_part = jnp.einsum("chij,cjhe->cihe", weights, value4, preferred_element_type=jnp.float32)
    tail_decay = jnp.exp(-(block_len - 1.0 - places)[:, None] * rates[None, :])
    decayed = (key4.astype(jnp.float32) * tail_decay[None, :, :, None]).astype(jnp.bfloat16)
    states = jnp.einsum("cjhd,cjhe->chde", decayed, value4, preferred_element_type=jnp.float32)
    passing = jnp.exp(-block_len * rates)[:, None, None]

    def advance(carried, fresh):
        return (carried * passing + fresh, carried)

    _, before = lax.scan(advance, jnp.zeros((head_count, width_k, width_v), jnp.float32), states)
    onset_decay = jnp.exp(-(places + 1.0)[:, None] * rates[None, :])
    cross_part = (
        jnp.einsum(
            "cihd,chde->cihe", query4.astype(jnp.float32), before, precision=lax.Precision.HIGHEST
        )
        * onset_decay[None, :, :, None]
    )
    return (inner_part + cross_part).reshape(length, head_count, width_v)


def head_norm(retained):
    average = jnp.mean(retained, axis=-1, keepdims=True)
    centered = retained - average
    return centered * lax.rsqrt(jnp.mean(centered * centered, axis=-1, keepdims=True) + epsilon)


def causal_taps(matrix, kernel_w):
    length = matrix.shape[0]
    padded = jnp.pad(matrix.astype(jnp.float32), ((KERNEL - 1, 0), (0, 0)))
    total = jnp.zeros((length, matrix.shape[1]), jnp.float32)
    for tap_idx in range(KERNEL):
        total = total + kernel_w[tap_idx][None, :] * padded[tap_idx : tap_idx + length]
    return total


def sum_over_tp(partial, tp_rank):
    rows = partial.shape[0] // 2
    mine = lax.dynamic_slice_in_dim(partial, tp_rank * rows, rows, 0)
    theirs = lax.dynamic_slice_in_dim(partial, (1 - tp_rank) * rows, rows, 0)
    got = lax.ppermute(theirs, "tp", [(0, 1), (1, 0)])
    return mine.astype(jnp.float32) + got.astype(jnp.float32)


def share_over_tp(matrix, tp_rank):
    got = lax.ppermute(matrix, "tp", [(0, 1), (1, 0)])
    first = tp_rank == 0
    return jnp.concatenate([jnp.where(first, matrix, got), jnp.where(first, got, matrix)], axis=0)


def body(
    sizes,
    tokens,
    mix_gain,
    w_query,
    w_key,
    w_value,
    w_out,
    ffn_gain,
    w_ffgate,
    w_ffup,
    conv_gate,
    conv_up,
    w_down,
):
    tp_rank = lax.axis_index("tp")
    heads_here = w_query.shape[1] // DK
    qk_cols = w_query.shape[1]
    qkv_shard = jnp.concatenate([w_query, w_key, w_value], axis=1)
    both, (qkv_w, out_full, gate_w, up_w, down_full) = gather_all(
        sizes,
        tokens,
        ((qkv_shard, False), (w_out, True), (w_ffgate, False), (w_ffup, False), (w_down, True)),
    )
    pieces = rms_rows(both, mix_gain)
    joined = jnp.dot(pieces, qkv_w, preferred_element_type=jnp.float32).astype(jnp.bfloat16)
    length = joined.shape[0]
    query = joined[:, :qk_cols].reshape(length, heads_here, DK)
    key = joined[:, qk_cols : 2 * qk_cols].reshape(length, heads_here, DK)
    value = joined[:, 2 * qk_cols :].reshape(length, heads_here, DV)
    rot_query = rotate_heads(query).astype(jnp.bfloat16)
    rot_key = (rotate_heads(key) * DK ** (-0.5)).astype(jnp.bfloat16)
    head_ids = (tp_rank * heads_here + jnp.arange(heads_here, dtype=jnp.int32)).astype(jnp.float32)
    rates = 1.0 / 16.0 * (32.0 / LENGTH) ** (head_ids / (HEADS - 1))
    retained = retain_blocks(rot_query, rot_key, value, rates, BLOCK)
    hidden = head_norm(retained).reshape(length, heads_here * DV).astype(jnp.bfloat16)
    mix_sum = sum_over_tp(
        jnp.dot(hidden, out_full, preferred_element_type=jnp.float32).astype(jnp.bfloat16), tp_rank
    )
    resid = (tokens.astype(jnp.float32) + mix_sum).astype(jnp.bfloat16)
    normed_ffn = rms_rows(resid, ffn_gain)
    ff_here = w_ffgate.shape[1]
    pieces = share_over_tp(normed_ffn, tp_rank)
    gate_pre = jnp.dot(pieces, gate_w, preferred_element_type=jnp.float32).astype(jnp.bfloat16)
    up_pre = jnp.dot(pieces, up_w, preferred_element_type=jnp.float32).astype(jnp.bfloat16)
    gate_taps = lax.dynamic_slice_in_dim(conv_gate, tp_rank * ff_here, ff_here, 1)
    up_taps = lax.dynamic_slice_in_dim(conv_up, tp_rank * ff_here, ff_here, 1)
    activ = (jax.nn.silu(causal_taps(gate_pre, gate_taps)) * causal_taps(up_pre, up_taps)).astype(
        jnp.bfloat16
    )
    ffn_sum = sum_over_tp(
        jnp.dot(activ, down_full, preferred_element_type=jnp.float32).astype(jnp.bfloat16), tp_rank
    )
    return (resid.astype(jnp.float32) + ffn_sum).astype(jnp.bfloat16)


def solution(mesh):
    sizes = (mesh.shape["rep"], mesh.shape["fs"], mesh.shape["tp"])
    placed = (
        P(("rep", "fs", "tp"), None),
        P(),
        P("fs", "tp"),
        P("fs", "tp"),
        P("fs", "tp"),
        P("tp", "fs"),
        P(),
        P("fs", "tp"),
        P("fs", "tp"),
        P(),
        P(),
        P("tp", "fs"),
    )
    return jax.shard_map(
        functools.partial(body, sizes),
        mesh=mesh, in_specs=placed, out_specs=P(("rep", "fs", "tp"), None), check_vma=False
    )
```

```python
import functools

import jax
import jax.numpy as jnp
from jax import lax
from jax.experimental import pallas as pl
from jax.experimental.pallas import tpu as pltpu
from jax.sharding import PartitionSpec as P

HEADS = 4
DK = 128
DV = 256
KERNEL = 3
BLOCK = 128
LENGTH = 1024
MESH = pl.DeviceIdType.MESH
ROWS, COLS = "rows", "cols"


epsilon = 1e-06


def gather_kernel(sizes, kinds, *refs):
    reps, fs, tps = sizes
    count = len(kinds)
    tokens = refs[0]
    shards = refs[1 : 1 + count]
    gain, cosine, sine, inside, tail, onset, passing = refs[1 + count : 8 + count]
    hidden = refs[8 + count]
    fulls = (refs[8 + 2 * count],) + tuple(refs[9 + count : 8 + 2 * count])
    (both, state, tok_sems, own_sems, up_send, up_recv, down_send, down_recv, y_send, y_recv, x_send, x_recv) = refs[
        9 + 2 * count :
    ]
    depth = fs // 2
    rep = lax.axis_index("rep")
    place = lax.axis_index("fs")
    core = lax.axis_index("tp")
    z = place // 2
    y = lax.rem(place, 2)
    above = {"fs": lax.rem(place + 2, fs)}
    below = {"fs": lax.rem(place + fs - 2, fs)}
    beside = {"fs": z * 2 + 1 - y}
    twin = {"rep": 1 - rep}
    other = {"tp": 1 - core}

    barrier = pltpu.get_barrier_semaphore()

    def greet(device):
        pl.semaphore_signal(barrier, inc=1, device_id=device, device_id_type=MESH)

    greet(beside)
    greet(twin)
    greet(other)
    pl.when(z < depth - 1)(lambda: greet(above))
    pl.when(z > 0)(lambda: greet(below))
    at_end = (z == 0) | (z == depth - 1)
    pl.when(at_end)(lambda: pl.semaphore_wait(barrier, 4))
    pl.when(jnp.logical_not(at_end))(lambda: pl.semaphore_wait(barrier, 5))

    def slot(p, owner, start, size):
        rows, cols = shards[p].shape
        start = pl.multiple_of(start, 16)
        if kinds[p] == COLS:
            return fulls[p].at[pl.ds(start, size), pl.ds(pl.multiple_of(owner * cols, 128), cols)]
        return fulls[p].at[pl.ds(pl.multiple_of(owner * rows, 16) + start, size)]

    def spans(p):
        rows = shards[p].shape[0]
        third = rows * 5 // 16 // 16 * 16
        return third, rows - third

    def piece(p, owner, own):
        third, most = spans(p)
        start = rep * third
        src = shards[p].at[pl.ds(pl.multiple_of(start, 16), most)] if own else slot(p, owner, start, most)
        return src, slot(p, owner, start, most)

    def copy(src, dst, send, recv, device):
        return pltpu.make_async_remote_copy(
            src_ref=src, dst_ref=dst, send_sem=send, recv_sem=recv, device_id=device, device_id_type=MESH
        )

    def clip(value):
        return jnp.minimum(jnp.maximum(value, 0), depth - 1)

    def up(p, s):
        src, dst = piece(p, clip(z - s) * 2 + y, s == 0)
        return copy(src, dst, up_send.at[p, s], up_recv.at[p, s], above)

    def down(p, s):
        src, dst = piece(p, clip(z + s) * 2 + y, s == 0)
        return copy(src, dst, down_send.at[p, s], down_recv.at[p, s], below)

    def up_in(p, s):
        dst = piece(p, clip(z - 1 - s) * 2 + y, False)[1]
        return copy(dst, dst, up_send.at[p, s], up_recv.at[p, s], above)

    def down_in(p, s):
        dst = piece(p, clip(z + 1 + s) * 2 + y, False)[1]
        return copy(dst, dst, down_send.at[p, s], down_recv.at[p, s], below)

    def level(k):
        return z if k == 0 else (clip(z - k) if k < depth else clip(z + k - depth + 1))

    def valid(k):
        return z >= 0 if k == 0 else (z - k >= 0 if k < depth else z + k - depth + 1 < depth)

    def y_copy(p, k):
        src, dst = piece(p, level(k) * 2 + y, k == 0)
        return copy(src, dst, y_send.at[p, k], y_recv.at[p, k], beside)

    def y_in(p, k):
        dst = piece(p, level(k) * 2 + 1 - y, False)[1]
        return copy(dst, dst, y_send.at[p, k], y_recv.at[p, k], beside)

    kmax = 2 * depth - 1

    def x_copy(p, k, side, mine):
        third, most = spans(p)
        who = rep if mine else 1 - rep
        lane = y if side == 0 else 1 - y
        ref = slot(p, level(k) * 2 + lane, who * most, third)
        return copy(ref, ref, x_send.at[p, side * kmax + k], x_recv.at[p, side * kmax + k], twin)

    tok_rows = tokens.shape[0]
    here = both.at[pl.ds(pl.multiple_of(core * tok_rows, 16), tok_rows)]
    tok_out = copy(tokens, here, tok_sems.at[0], tok_sems.at[1], other)
    tok_out.start()
    tok_own = pltpu.make_async_copy(tokens, here, tok_sems.at[2])
    tok_own.start()
    owns = []
    for p in range(count):
        own = pltpu.make_async_copy(shards[p], slot(p, place, 0, shards[p].shape[0]), own_sems.at[p])
        own.start()
        owns.append(own)

    steps = depth - 1
    events = [(p, s) for p in range(count) for s in range(steps)]

    def start_z(p, s):
        pl.when((z - s >= 0) & (z < depth - 1))(lambda: up(p, s).start())
        pl.when((z + s <= depth - 1) & (z > 0))(lambda: down(p, s).start())
        if s == 0:
            y_copy(p, 0).start()

    def take_z(p, s):
        ku, kd = s + 1, depth + s

        @pl.when(z - 1 - s >= 0)
        def _():
            up_in(p, s).wait_recv()

        @pl.when(z + 1 + s <= depth - 1)
        def _():
            down_in(p, s).wait_recv()

    def spread(p, s):
        for k in (s + 1, depth + s):

            @pl.when(valid(k))
            def _():
                y_copy(p, k).start()
                x_copy(p, k, 0, True).start()

    def take_y(p, k):
        @pl.when(valid(k))
        def _():
            y_in(p, k).wait_recv()
            x_copy(p, k, 1, True).start()

    def finish_y(p, s):
        if s == 0:
            take_y(p, 0)
        take_y(p, s + 1)
        take_y(p, depth + s)

    heads = state.shape[0]

    def ready():
        for k in range(kmax):

            @pl.when(valid(k))
            def _():
                if k > 0:
                    x_copy(0, k, 0, False).wait_recv()
                x_copy(0, k, 1, False).wait_recv()

        owns[0].wait()
        tok_own.wait()
        tok_out.wait()
        state[...] = jnp.zeros_like(state)

    def attend(c):
        span = pl.ds(c * BLOCK, BLOCK)
        values = both[span, :].astype(jnp.float32)
        factor = lax.rsqrt(jnp.mean(values * values, axis=-1, keepdims=True) + epsilon)
        normed = (values * factor * gain[...]).astype(jnp.bfloat16)
        joined = jnp.dot(normed, fulls[0][...], preferred_element_type=jnp.float32).astype(jnp.bfloat16)
        cos, sin = cosine[span, :], sine[span, :]

        def rotate(matrix):
            wide = matrix.astype(jnp.float32)
            return wide * cos + pltpu.roll(wide, DK // 2, 1) * sin

        for h in range(heads):
            query = rotate(joined[:, h * DK : (h + 1) * DK]).astype(jnp.bfloat16)
            key = joined[:, (heads + h) * DK : (heads + h + 1) * DK]
            key = (rotate(key) * DK ** (-0.5)).astype(jnp.bfloat16)
            first = 2 * heads * DK + h * DV
            value = joined[:, first : first + DV]
            scores = lax.dot_general(query, key, (((1,), (1,)), ((), ())), preferred_element_type=jnp.float32)
            weights = (scores * inside[h]).astype(jnp.bfloat16)
            inner = jnp.dot(weights, value, preferred_element_type=jnp.float32)
            cross = jnp.dot(
                query.astype(jnp.float32),
                state[h],
                precision=lax.Precision.HIGHEST,
                preferred_element_type=jnp.float32,
            )
            retained = inner + cross * onset[h]
            decayed = (key.astype(jnp.float32) * tail[h]).astype(jnp.bfloat16)
            fresh = lax.dot_general(decayed, value, (((0,), (0,)), ((), ())), preferred_element_type=jnp.float32)
            state[h] = state[h] * passing[h] + fresh
            hidden[span, h * DV : (h + 1) * DV] = head_norm(retained).astype(jnp.bfloat16)

    lag = 2
    first_block = steps + lag + 1
    blocks = both.shape[0] // BLOCK
    total = len(events)
    start_z(*events[0])
    for e in range(max(total + lag, first_block + blocks)):
        if e < total:
            p, s = events[e]
            if s == steps - 2 and p + 1 < count:
                start_z(p + 1, 0)
            take_z(p, s)
            if s + 1 < steps:
                start_z(p, s + 1)
            spread(p, s)
        if lag <= e < total + lag:
            finish_y(*events[e - lag])
        if e == first_block:
            ready()
        if first_block <= e < first_block + blocks:
            attend(e - first_block)

    for p in range(count):
        for k in range(kmax):

            @pl.when(valid(k))
            def _():
                if k > 0:
                    if p > 0:
                        x_copy(p, k, 0, False).wait_recv()
                    x_copy(p, k, 0, True).wait_send()
                if p > 0:
                    x_copy(p, k, 1, False).wait_recv()
                x_copy(p, k, 1, True).wait_send()
                y_copy(p, k).wait_send()

        for s in range(steps):
            pl.when((z - s >= 0) & (z < depth - 1))(lambda: up(p, s).wait_send())
            pl.when((z + s <= depth - 1) & (z > 0))(lambda: down(p, s).wait_send())
    for own in owns[1:]:
        own.wait()


def gather_all(sizes, tokens, shards, tables):
    fs = sizes[1]
    kinds = []
    length = tokens.shape[0] * 2
    heads = tables[3].shape[0]
    outs = [jax.ShapeDtypeStruct((length, heads * DV), jnp.bfloat16)]
    for shard, by_cols in shards:
        rows, cols = shard.shape
        side = by_cols and cols % 128 == 0
        kinds.append(COLS if side else ROWS)
        outs.append(jax.ShapeDtypeStruct((rows, cols * fs) if side else (rows * fs, cols), shard.dtype))
    count, depth = len(shards), fs // 2
    dma = pltpu.SemaphoreType.DMA
    vmem = pl.BlockSpec(memory_space=pltpu.VMEM)
    anywhere = pl.BlockSpec(memory_space=pl.ANY)
    got = pl.pallas_call(
        functools.partial(gather_kernel, sizes, tuple(kinds)),
        out_shape=outs[:1] + outs[2:],
        in_specs=[vmem] * (count + 1 + len(tables)),
        out_specs=[vmem] + [anywhere] * (count - 1),
        scratch_shapes=[
            pltpu.VMEM(outs[1].shape, outs[1].dtype),
            pltpu.VMEM((length, tokens.shape[1]), tokens.dtype),
            pltpu.VMEM((heads, DK, DV), jnp.float32),
            dma((3,)),
            dma((count,)),
        ]
        + [dma((count, depth - 1))] * 4
        + [dma((count, 2 * depth - 1))] * 2
        + [dma((count, 4 * depth - 2))] * 2,
        compiler_params=pltpu.CompilerParams(collective_id=0, has_side_effects=True),
    )(tokens, *[shard for shard, _ in shards], *tables)
    fulls = []
    for full, (shard, by_cols), kind in zip(got[1:], shards[1:], kinds[1:]):
        if by_cols and kind == ROWS:
            rows, cols = shard.shape
            full = full.reshape(fs, rows, cols).transpose(1, 0, 2).reshape(rows, fs * cols)
        fulls.append(full)
    return got[0], fulls


def rms_rows(matrix, scale_vec):
    values = matrix.astype(jnp.float32)
    factor = lax.rsqrt(jnp.mean(values * values, axis=-1, keepdims=True) + epsilon)
    return (values * factor * scale_vec).astype(jnp.bfloat16)


def rotation(length):
    half_width = DK // 2
    inverse = 10000.0 ** (-jnp.arange(half_width, dtype=jnp.float32) * 2.0 / (2 * half_width))
    angles = jnp.arange(length, dtype=jnp.float32)[:, None] * inverse[None, :]
    cosine, sine = jnp.cos(angles), jnp.sin(angles)
    return jnp.concatenate([cosine, cosine], axis=1), jnp.concatenate([-sine, sine], axis=1)


def decays(rates, block_len):
    heads = rates.shape[0]
    places = jnp.arange(block_len, dtype=jnp.float32)
    spacing = places[:, None] - places[None, :]
    inside = jnp.where(
        spacing[None] >= 0, jnp.exp(-jnp.maximum(spacing, 0.0)[None] * rates[:, None, None]), 0.0
    )
    tail = jnp.exp(-(block_len - 1.0 - places)[None, :, None] * rates[:, None, None])
    onset = jnp.exp(-(places + 1.0)[None, :, None] * rates[:, None, None])
    passing = jnp.exp(-block_len * rates)[:, None, None]
    return (
        inside,
        jnp.broadcast_to(tail, (heads, block_len, DK)),
        jnp.broadcast_to(onset, (heads, block_len, DV)),
        jnp.broadcast_to(passing, (heads, 1, DV)),
    )


def head_norm(retained):
    average = jnp.mean(retained, axis=-1, keepdims=True)
    centered = retained - average
    return centered * lax.rsqrt(jnp.mean(centered * centered, axis=-1, keepdims=True) + epsilon)


def causal_taps(matrix, kernel_w):
    length = matrix.shape[0]
    padded = jnp.pad(matrix.astype(jnp.float32), ((KERNEL - 1, 0), (0, 0)))
    total = jnp.zeros((length, matrix.shape[1]), jnp.float32)
    for tap_idx in range(KERNEL):
        total = total + kernel_w[tap_idx][None, :] * padded[tap_idx : tap_idx + length]
    return total


def sum_over_tp(partial, tp_rank):
    rows = partial.shape[0] // 2
    mine = lax.dynamic_slice_in_dim(partial, tp_rank * rows, rows, 0)
    theirs = lax.dynamic_slice_in_dim(partial, (1 - tp_rank) * rows, rows, 0)
    got = lax.ppermute(theirs, "tp", [(0, 1), (1, 0)])
    return mine.astype(jnp.float32) + got.astype(jnp.float32)


def share_over_tp(matrix, tp_rank):
    got = lax.ppermute(matrix, "tp", [(0, 1), (1, 0)])
    first = tp_rank == 0
    return jnp.concatenate([jnp.where(first, matrix, got), jnp.where(first, got, matrix)], axis=0)


def body(
    sizes,
    tokens,
    mix_gain,
    w_query,
    w_key,
    w_value,
    w_out,
    ffn_gain,
    w_ffgate,
    w_ffup,
    conv_gate,
    conv_up,
    w_down,
):
    tp_rank = lax.axis_index("tp")
    heads_here = w_query.shape[1] // DK
    qk_cols = w_query.shape[1]
    qkv_shard = jnp.concatenate([w_query, w_key, w_value], axis=1)
    length = tokens.shape[0] * 2
    head_ids = (tp_rank * heads_here + jnp.arange(heads_here, dtype=jnp.int32)).astype(jnp.float32)
    rates = 1.0 / 16.0 * (32.0 / LENGTH) ** (head_ids / (HEADS - 1))
    hidden, (out_full, gate_w, up_w, down_full) = gather_all(
        sizes,
        tokens,
        ((qkv_shard, False), (w_out, True), (w_ffgate, False), (w_ffup, False), (w_down, True)),
        (mix_gain[None, :],) + rotation(length) + decays(rates, BLOCK),
    )
    mix_sum = sum_over_tp(
        jnp.dot(hidden, out_full, preferred_element_type=jnp.float32).astype(jnp.bfloat16), tp_rank
    )
    resid = (tokens.astype(jnp.float32) + mix_sum).astype(jnp.bfloat16)
    normed_ffn = rms_rows(resid, ffn_gain)
    ff_here = w_ffgate.shape[1]
    pieces = share_over_tp(normed_ffn, tp_rank)
    gate_pre = jnp.dot(pieces, gate_w, preferred_element_type=jnp.float32).astype(jnp.bfloat16)
    up_pre = jnp.dot(pieces, up_w, preferred_element_type=jnp.float32).astype(jnp.bfloat16)
    gate_taps = lax.dynamic_slice_in_dim(conv_gate, tp_rank * ff_here, ff_here, 1)
    up_taps = lax.dynamic_slice_in_dim(conv_up, tp_rank * ff_here, ff_here, 1)
    activ = (jax.nn.silu(causal_taps(gate_pre, gate_taps)) * causal_taps(up_pre, up_taps)).astype(
        jnp.bfloat16
    )
    ffn_sum = sum_over_tp(
        jnp.dot(activ, down_full, preferred_element_type=jnp.float32).astype(jnp.bfloat16), tp_rank
    )
    return (resid.astype(jnp.float32) + ffn_sum).astype(jnp.bfloat16)


def solution(mesh):
    sizes = (mesh.shape["rep"], mesh.shape["fs"], mesh.shape["tp"])
    placed = (
        P(("rep", "fs", "tp"), None),
        P(),
        P("fs", "tp"),
        P("fs", "tp"),
        P("fs", "tp"),
        P("tp", "fs"),
        P(),
        P("fs", "tp"),
        P("fs", "tp"),
        P(),
        P(),
        P("tp", "fs"),
    )
    return jax.shard_map(
        functools.partial(body, sizes),
        mesh=mesh, in_specs=placed, out_specs=P(("rep", "fs", "tp"), None), check_vma=False
    )
```

```python
import functools

import jax
import jax.numpy as jnp
from jax import lax
from jax.experimental import pallas as pl
from jax.experimental.pallas import tpu as pltpu
from jax.sharding import PartitionSpec as P

HEADS = 4
DK = 128
DV = 256
KERNEL = 3
BLOCK = 128
LENGTH = 1024
MESH = pl.DeviceIdType.MESH
ROWS, COLS = "rows", "cols"


epsilon = 1e-06


def gather_kernel(sizes, kinds, *refs):
    reps, fs, tps = sizes
    count = len(kinds)
    tokens = refs[0]
    shards = refs[1 : 1 + count]
    gain, cosine, sine, inside, tail, onset, passing = refs[1 + count : 8 + count]
    hidden = refs[8 + count]
    fulls = (refs[8 + 2 * count],) + tuple(refs[9 + count : 8 + 2 * count])
    (both, state, tok_sems, own_sems, up_send, up_recv, down_send, down_recv, y_send, y_recv, x_send, x_recv) = refs[
        9 + 2 * count :
    ]
    depth = fs // 2
    rep = lax.axis_index("rep")
    place = lax.axis_index("fs")
    core = lax.axis_index("tp")
    z = place // 2
    y = lax.rem(place, 2)
    above = {"fs": lax.rem(place + 2, fs)}
    below = {"fs": lax.rem(place + fs - 2, fs)}
    beside = {"fs": z * 2 + 1 - y}
    twin = {"rep": 1 - rep}
    other = {"tp": 1 - core}

    barrier = pltpu.get_barrier_semaphore()

    def greet(device):
        pl.semaphore_signal(barrier, inc=1, device_id=device, device_id_type=MESH)

    greet(beside)
    greet(twin)
    greet(other)
    pl.when(z < depth - 1)(lambda: greet(above))
    pl.when(z > 0)(lambda: greet(below))
    at_end = (z == 0) | (z == depth - 1)
    pl.when(at_end)(lambda: pl.semaphore_wait(barrier, 4))
    pl.when(jnp.logical_not(at_end))(lambda: pl.semaphore_wait(barrier, 5))

    def slot(p, owner, start, size):
        rows, cols = shards[p].shape
        start = pl.multiple_of(start, 16)
        if kinds[p] == COLS:
            return fulls[p].at[pl.ds(start, size), pl.ds(pl.multiple_of(owner * cols, 128), cols)]
        return fulls[p].at[pl.ds(pl.multiple_of(owner * rows, 16) + start, size)]

    def spans(p):
        rows = shards[p].shape[0]
        share = 6 if p < count - 1 else 4
        third = rows * share // 16 // 16 * 16
        return third, rows - third

    def piece(p, owner, own):
        third, most = spans(p)
        start = rep * third
        src = shards[p].at[pl.ds(pl.multiple_of(start, 16), most)] if own else slot(p, owner, start, most)
        return src, slot(p, owner, start, most)

    def copy(src, dst, send, recv, device):
        return pltpu.make_async_remote_copy(
            src_ref=src, dst_ref=dst, send_sem=send, recv_sem=recv, device_id=device, device_id_type=MESH
        )

    def clip(value):
        return jnp.minimum(jnp.maximum(value, 0), depth - 1)

    def up(p, s):
        src, dst = piece(p, clip(z - s) * 2 + y, s == 0)
        return copy(src, dst, up_send.at[p, s], up_recv.at[p, s], above)

    def down(p, s):
        src, dst = piece(p, clip(z + s) * 2 + y, s == 0)
        return copy(src, dst, down_send.at[p, s], down_recv.at[p, s], below)

    def up_in(p, s):
        dst = piece(p, clip(z - 1 - s) * 2 + y, False)[1]
        return copy(dst, dst, up_send.at[p, s], up_recv.at[p, s], above)

    def down_in(p, s):
        dst = piece(p, clip(z + 1 + s) * 2 + y, False)[1]
        return copy(dst, dst, down_send.at[p, s], down_recv.at[p, s], below)

    def level(k):
        return z if k == 0 else (clip(z - k) if k < depth else clip(z + k - depth + 1))

    def valid(k):
        return z >= 0 if k == 0 else (z - k >= 0 if k < depth else z + k - depth + 1 < depth)

    def y_copy(p, k):
        src, dst = piece(p, level(k) * 2 + y, k == 0)
        return copy(src, dst, y_send.at[p, k], y_recv.at[p, k], beside)

    def y_in(p, k):
        dst = piece(p, level(k) * 2 + 1 - y, False)[1]
        return copy(dst, dst, y_send.at[p, k], y_recv.at[p, k], beside)

    kmax = 2 * depth - 1

    def x_copy(p, k, side, mine):
        third, most = spans(p)
        who = rep if mine else 1 - rep
        lane = y if side == 0 else 1 - y
        ref = slot(p, level(k) * 2 + lane, who * most, third)
        return copy(ref, ref, x_send.at[p, side * kmax + k], x_recv.at[p, side * kmax + k], twin)

    tok_rows = tokens.shape[0]
    here = both.at[pl.ds(pl.multiple_of(core * tok_rows, 16), tok_rows)]
    tok_out = copy(tokens, here, tok_sems.at[0], tok_sems.at[1], other)
    tok_out.start()
    tok_own = pltpu.make_async_copy(tokens, here, tok_sems.at[2])
    tok_own.start()
    owns = []
    for p in range(count):
        own = pltpu.make_async_copy(shards[p], slot(p, place, 0, shards[p].shape[0]), own_sems.at[p])
        own.start()
        owns.append(own)

    steps = depth - 1
    events = [(p, s) for p in range(count) for s in range(steps)]

    def start_z(p, s):
        pl.when((z - s >= 0) & (z < depth - 1))(lambda: up(p, s).start())
        pl.when((z + s <= depth - 1) & (z > 0))(lambda: down(p, s).start())
        if s == 0:
            y_copy(p, 0).start()

    def take_z(p, s):
        ku, kd = s + 1, depth + s

        @pl.when(z - 1 - s >= 0)
        def _():
            up_in(p, s).wait_recv()

        @pl.when(z + 1 + s <= depth - 1)
        def _():
            down_in(p, s).wait_recv()

    def spread(p, s):
        for k in (s + 1, depth + s):

            @pl.when(valid(k))
            def _():
                y_copy(p, k).start()
                x_copy(p, k, 0, True).start()

    def take_y(p, k):
        @pl.when(valid(k))
        def _():
            y_in(p, k).wait_recv()
            x_copy(p, k, 1, True).start()

    def finish_y(p, s):
        if s == 0:
            take_y(p, 0)
        take_y(p, s + 1)
        take_y(p, depth + s)

    heads = state.shape[0]

    def ready():
        for k in range(kmax):

            @pl.when(valid(k))
            def _():
                if k > 0:
                    x_copy(0, k, 0, False).wait_recv()
                x_copy(0, k, 1, False).wait_recv()

        owns[0].wait()
        tok_own.wait()
        tok_out.wait()
        state[...] = jnp.zeros_like(state)

    def attend(c):
        span = pl.ds(c * BLOCK, BLOCK)
        values = both[span, :].astype(jnp.float32)
        factor = lax.rsqrt(jnp.mean(values * values, axis=-1, keepdims=True) + epsilon)
        normed = (values * factor * gain[...]).astype(jnp.bfloat16)
        joined = jnp.dot(normed, fulls[0][...], preferred_element_type=jnp.float32).astype(jnp.bfloat16)
        cos, sin = cosine[span, :], sine[span, :]

        def rotate(matrix):
            wide = matrix.astype(jnp.float32)
            return wide * cos + pltpu.roll(wide, DK // 2, 1) * sin

        for h in range(heads):
            query = rotate(joined[:, h * DK : (h + 1) * DK]).astype(jnp.bfloat16)
            key = joined[:, (heads + h) * DK : (heads + h + 1) * DK]
            key = (rotate(key) * DK ** (-0.5)).astype(jnp.bfloat16)
            first = 2 * heads * DK + h * DV
            value = joined[:, first : first + DV]
            scores = lax.dot_general(query, key, (((1,), (1,)), ((), ())), preferred_element_type=jnp.float32)
            weights = (scores * inside[h]).astype(jnp.bfloat16)
            inner = jnp.dot(weights, value, preferred_element_type=jnp.float32)
            cross = jnp.dot(
                query.astype(jnp.float32),
                state[h],
                precision=lax.Precision.HIGHEST,
                preferred_element_type=jnp.float32,
            )
            retained = inner + cross * onset[h]
            decayed = (key.astype(jnp.float32) * tail[h]).astype(jnp.bfloat16)
            fresh = lax.dot_general(decayed, value, (((0,), (0,)), ((), ())), preferred_element_type=jnp.float32)
            state[h] = state[h] * passing[h] + fresh
            hidden[span, h * DV : (h + 1) * DV] = head_norm(retained).astype(jnp.bfloat16)

    lag = 2
    first_block = steps + lag + 1
    blocks = both.shape[0] // BLOCK
    total = len(events)
    start_z(*events[0])
    for e in range(max(total + lag, first_block + blocks)):
        if e < total:
            p, s = events[e]
            if s == steps - 2 and p + 1 < count:
                start_z(p + 1, 0)
            take_z(p, s)
            if s + 1 < steps:
                start_z(p, s + 1)
            spread(p, s)
        if lag <= e < total + lag:
            finish_y(*events[e - lag])
        if e == first_block:
            ready()
        if first_block <= e < first_block + blocks:
            attend(e - first_block)

    for p in range(count):
        for k in range(kmax):

            @pl.when(valid(k))
            def _():
                if k > 0:
                    if p > 0:
                        x_copy(p, k, 0, False).wait_recv()
                    x_copy(p, k, 0, True).wait_send()
                if p > 0:
                    x_copy(p, k, 1, False).wait_recv()
                x_copy(p, k, 1, True).wait_send()
                y_copy(p, k).wait_send()

        for s in range(steps):
            pl.when((z - s >= 0) & (z < depth - 1))(lambda: up(p, s).wait_send())
            pl.when((z + s <= depth - 1) & (z > 0))(lambda: down(p, s).wait_send())
    for own in owns[1:]:
        own.wait()


def gather_all(sizes, tokens, shards, tables):
    fs = sizes[1]
    kinds = []
    length = tokens.shape[0] * 2
    heads = tables[3].shape[0]
    outs = [jax.ShapeDtypeStruct((length, heads * DV), jnp.bfloat16)]
    for shard, by_cols in shards:
        rows, cols = shard.shape
        side = by_cols and cols % 128 == 0
        kinds.append(COLS if side else ROWS)
        outs.append(jax.ShapeDtypeStruct((rows, cols * fs) if side else (rows * fs, cols), shard.dtype))
    count, depth = len(shards), fs // 2
    dma = pltpu.SemaphoreType.DMA
    vmem = pl.BlockSpec(memory_space=pltpu.VMEM)
    anywhere = pl.BlockSpec(memory_space=pl.ANY)
    got = pl.pallas_call(
        functools.partial(gather_kernel, sizes, tuple(kinds)),
        out_shape=outs[:1] + outs[2:],
        in_specs=[vmem] * (count + 1 + len(tables)),
        out_specs=[vmem] + [anywhere] * (count - 1),
        scratch_shapes=[
            pltpu.VMEM(outs[1].shape, outs[1].dtype),
            pltpu.VMEM((length, tokens.shape[1]), tokens.dtype),
            pltpu.VMEM((heads, DK, DV), jnp.float32),
            dma((3,)),
            dma((count,)),
        ]
        + [dma((count, depth - 1))] * 4
        + [dma((count, 2 * depth - 1))] * 2
        + [dma((count, 4 * depth - 2))] * 2,
        compiler_params=pltpu.CompilerParams(collective_id=0, has_side_effects=True),
    )(tokens, *[shard for shard, _ in shards], *tables)
    fulls = []
    for full, (shard, by_cols), kind in zip(got[1:], shards[1:], kinds[1:]):
        if by_cols and kind == ROWS:
            rows, cols = shard.shape
            full = full.reshape(fs, rows, cols).transpose(1, 0, 2).reshape(rows, fs * cols)
        fulls.append(full)
    return got[0], fulls


def rms_rows(matrix, scale_vec):
    values = matrix.astype(jnp.float32)
    factor = lax.rsqrt(jnp.mean(values * values, axis=-1, keepdims=True) + epsilon)
    return (values * factor * scale_vec).astype(jnp.bfloat16)


def rotation(length):
    half_width = DK // 2
    inverse = 10000.0 ** (-jnp.arange(half_width, dtype=jnp.float32) * 2.0 / (2 * half_width))
    angles = jnp.arange(length, dtype=jnp.float32)[:, None] * inverse[None, :]
    cosine, sine = jnp.cos(angles), jnp.sin(angles)
    return jnp.concatenate([cosine, cosine], axis=1), jnp.concatenate([-sine, sine], axis=1)


def decays(rates, block_len):
    heads = rates.shape[0]
    places = jnp.arange(block_len, dtype=jnp.float32)
    spacing = places[:, None] - places[None, :]
    inside = jnp.where(
        spacing[None] >= 0, jnp.exp(-jnp.maximum(spacing, 0.0)[None] * rates[:, None, None]), 0.0
    )
    tail = jnp.exp(-(block_len - 1.0 - places)[None, :, None] * rates[:, None, None])
    onset = jnp.exp(-(places + 1.0)[None, :, None] * rates[:, None, None])
    passing = jnp.exp(-block_len * rates)[:, None, None]
    return (
        inside,
        jnp.broadcast_to(tail, (heads, block_len, DK)),
        jnp.broadcast_to(onset, (heads, block_len, DV)),
        jnp.broadcast_to(passing, (heads, 1, DV)),
    )


def head_norm(retained):
    average = jnp.mean(retained, axis=-1, keepdims=True)
    centered = retained - average
    return centered * lax.rsqrt(jnp.mean(centered * centered, axis=-1, keepdims=True) + epsilon)


def causal_taps(matrix, kernel_w):
    length = matrix.shape[0]
    padded = jnp.pad(matrix.astype(jnp.float32), ((KERNEL - 1, 0), (0, 0)))
    total = jnp.zeros((length, matrix.shape[1]), jnp.float32)
    for tap_idx in range(KERNEL):
        total = total + kernel_w[tap_idx][None, :] * padded[tap_idx : tap_idx + length]
    return total


def sum_over_tp(partial, tp_rank):
    rows = partial.shape[0] // 2
    mine = lax.dynamic_slice_in_dim(partial, tp_rank * rows, rows, 0)
    theirs = lax.dynamic_slice_in_dim(partial, (1 - tp_rank) * rows, rows, 0)
    got = lax.ppermute(theirs, "tp", [(0, 1), (1, 0)])
    return mine.astype(jnp.float32) + got.astype(jnp.float32)


def share_over_tp(matrix, tp_rank):
    got = lax.ppermute(matrix, "tp", [(0, 1), (1, 0)])
    first = tp_rank == 0
    return jnp.concatenate([jnp.where(first, matrix, got), jnp.where(first, got, matrix)], axis=0)


def body(
    sizes,
    tokens,
    mix_gain,
    w_query,
    w_key,
    w_value,
    w_out,
    ffn_gain,
    w_ffgate,
    w_ffup,
    conv_gate,
    conv_up,
    w_down,
):
    tp_rank = lax.axis_index("tp")
    heads_here = w_query.shape[1] // DK
    qk_cols = w_query.shape[1]
    qkv_shard = jnp.concatenate([w_query, w_key, w_value], axis=1)
    length = tokens.shape[0] * 2
    head_ids = (tp_rank * heads_here + jnp.arange(heads_here, dtype=jnp.int32)).astype(jnp.float32)
    rates = 1.0 / 16.0 * (32.0 / LENGTH) ** (head_ids / (HEADS - 1))
    hidden, (out_full, gate_w, up_w, down_full) = gather_all(
        sizes,
        tokens,
        ((qkv_shard, False), (w_out, True), (w_ffgate, False), (w_ffup, False), (w_down, True)),
        (mix_gain[None, :],) + rotation(length) + decays(rates, BLOCK),
    )
    mix_sum = sum_over_tp(
        jnp.dot(hidden, out_full, preferred_element_type=jnp.float32).astype(jnp.bfloat16), tp_rank
    )
    resid = (tokens.astype(jnp.float32) + mix_sum).astype(jnp.bfloat16)
    normed_ffn = rms_rows(resid, ffn_gain)
    ff_here = w_ffgate.shape[1]
    pieces = share_over_tp(normed_ffn, tp_rank)
    gate_pre = jnp.dot(pieces, gate_w, preferred_element_type=jnp.float32).astype(jnp.bfloat16)
    up_pre = jnp.dot(pieces, up_w, preferred_element_type=jnp.float32).astype(jnp.bfloat16)
    gate_pre, up_pre = lax.optimization_barrier((gate_pre, up_pre))
    gate_taps = lax.dynamic_slice_in_dim(conv_gate, tp_rank * ff_here, ff_here, 1)
    up_taps = lax.dynamic_slice_in_dim(conv_up, tp_rank * ff_here, ff_here, 1)
    activ = (jax.nn.silu(causal_taps(gate_pre, gate_taps)) * causal_taps(up_pre, up_taps)).astype(
        jnp.bfloat16
    )
    activ = lax.optimization_barrier(activ)
    ffn_sum = sum_over_tp(
        jnp.dot(activ, down_full, preferred_element_type=jnp.float32).astype(jnp.bfloat16), tp_rank
    )
    return (resid.astype(jnp.float32) + ffn_sum).astype(jnp.bfloat16)


def solution(mesh):
    sizes = (mesh.shape["rep"], mesh.shape["fs"], mesh.shape["tp"])
    placed = (
        P(("rep", "fs", "tp"), None),
        P(),
        P("fs", "tp"),
        P("fs", "tp"),
        P("fs", "tp"),
        P("tp", "fs"),
        P(),
        P("fs", "tp"),
        P("fs", "tp"),
        P(),
        P(),
        P("tp", "fs"),
    )
    return jax.shard_map(
        functools.partial(body, sizes),
        mesh=mesh, in_specs=placed, out_specs=P(("rep", "fs", "tp"), None), check_vma=False
    )
```
